32 devices in a mesh: sp: 8 (over z, y), tp: 4 (over x, core).
Axes of the slice: x: 2, y: 2, z: 4, core: 2. Of those that a mesh axis runs over, the one named last changes fastest.
Arguments:
- queries: bfloat16 [8192, 1024], P('sp', 'tp'), may hold values from -6 to 6
- keys: bfloat16 [8192, 1024], P('sp', 'tp'), may hold values from -6 to 6
- values: bfloat16 [8192, 1024], P('sp', 'tp'), may hold values from -6 to 6
- gates: bfloat16 [8192, 1024], P('sp', 'tp'), may hold values from -6 to 6
- log_decay: float32 [8192, 8], P('sp', 'tp'), may hold values from -1.6 to 0, as said below
- norm_gain: float32 [8, 128], P('tp'), may hold values from 0.1 to 1.9
- out_weight: bfloat16 [1024, 2048], P('tp'), may hold values from -0.1875 to 0.1875
- resid: bfloat16 [8192, 2048], P(('sp', 'tp')), may hold values from -6 to 6
- post_mix_gain: float32 [2048], replicated, may hold values from 0.1 to 1.9
- pre_ffn_gain: float32 [2048], replicated, may hold values from 0.1 to 1.9
- w_gate: bfloat16 [2048, 5632], P('sp', 'tp'), may hold values from -0.125 to 0.125
- w_up: bfloat16 [2048, 5632], P('sp', 'tp'), may hold values from -0.125 to 0.125
- w_down: bfloat16 [5632, 2048], P('tp', 'sp'), may hold values from -0.078125 to 0.078125
- post_ffn_gain: float32 [2048], replicated, may hold values from 0.1 to 1.9
Outputs:
- updated: bfloat16 [8192, 2048], P(('sp', 'tp'))
The draws below stay inside these ranges and needn't reach their ends.
Inputs may be any that keep to these rules, and one draw needn't show every extreme that they name: `log_decay`: every entry is negative.
All inputs are finite; a program needn't handle non-finite values.
Results may differ from the reference program's by a relative error of at most 0.02.
Values may be sent and summed in bfloat16 or wider, within the bound.
A program may use at most 128 MiB of HBM per device.

```python
import math
import jax
import jax.numpy as jnp
from jax import lax

D = 2048
RETENTION_HEADS = 8
HEAD_DIM = 128
FF = 5632
TOK_DEV = 1024
RET_W = 1024
BLOCK = 512
SEQUENCE_TOKENS = 8192
N_TP = 4


def draw_log_decay(key, part):
    random_child_keys = jax.random.split(jax.random.fold_in(key, 17), 6)
    fast_share = 0.5
    is_fast = jax.random.uniform(random_child_keys[0], (RETENTION_HEADS,), jnp.float32) < fast_share
    fast_rate = jax.random.uniform(random_child_keys[1], (RETENTION_HEADS,), jnp.float32, 0.08, 0.15)
    baseline_decay_rate = jnp.where(is_fast, fast_rate, 0.6 / SEQUENCE_TOKENS)
    span_count = SEQUENCE_TOKENS // TOK_DEV
    factor = jnp.exp(jax.random.uniform(random_child_keys[2], (span_count, RETENTION_HEADS), jnp.float32, math.log(0.4), math.log(1.6)))
    row_values = jnp.repeat(factor, TOK_DEV, axis=0)
    random_noise = jax.random.uniform(random_child_keys[3], (SEQUENCE_TOKENS, RETENTION_HEADS), jnp.float32, 0.5, 1.5)
    spike_position = jax.random.randint(random_child_keys[4], (2, RETENTION_HEADS), 0, SEQUENCE_TOKENS)
    spike_length = jnp.log(jax.random.uniform(random_child_keys[5], (2, RETENTION_HEADS), jnp.float32, 0.55, 0.8))
    token_positions = lax.broadcasted_iota(jnp.int32, (SEQUENCE_TOKENS, RETENTION_HEADS), 0)
    spike_events = jnp.where(token_positions == spike_position[0][None, :], spike_length[0][None, :], 0.0)
    spike_events = spike_events + jnp.where(token_positions == spike_position[1][None, :], spike_length[1][None, :], 0.0)
    return (-baseline_decay_rate[None, :] * row_values * random_noise + spike_events).astype(jnp.float32)


def steps_of(own_key, extent, shards, low, largest):
    loudness, own = 1.0, jax.random.fold_in(own_key, 6)
    for axis_at, blocks in shards:
        draws = jnp.exp(jax.random.uniform(jax.random.fold_in(own, axis_at), (blocks,), jnp.float32, low / len(shards), largest / len(shards)))
        loudness = loudness * jnp.repeat(draws, extent[axis_at] // blocks).reshape([-1 if axis == axis_at else 1 for axis in range(len(extent))])
    return loudness


def normal_values(own_key, shape, spread, reach, cuts=(), dtype=jnp.bfloat16):
    result = spread * jax.random.normal(own_key, shape, jnp.float32)
    if cuts:
        result = result * steps_of(own_key, shape, cuts, -0.22, 0.18)
    return jnp.clip(result, -reach, reach).astype(dtype)


def setup_inputs(seed: int = 0) -> dict:
    streams_of = jax.random.split(jax.random.key(seed), 15)
    return {
        "queries": normal_values(streams_of[0], (SEQUENCE_TOKENS, RET_W), 1.0, 6.0, ((0, 8), (1, 4))),
        "keys": normal_values(streams_of[1], (SEQUENCE_TOKENS, RET_W), 1.0, 6.0, ((0, 8), (1, 4))),
        "values": normal_values(streams_of[2], (SEQUENCE_TOKENS, RET_W), 1.0, 6.0, ((0, 8), (1, 4))),
        "gates": normal_values(streams_of[3], (SEQUENCE_TOKENS, RET_W), 1.0, 6.0, ((0, 8), (1, 4))),
        "log_decay": draw_log_decay(jax.random.fold_in(streams_of[14], 71), 0),
        "norm_gain": jnp.clip(1.0 + 0.18 * jax.random.normal(streams_of[5], (RETENTION_HEADS, HEAD_DIM), jnp.float32), 0.1, 1.9),
        "out_weight": normal_values(streams_of[6], (RET_W, D), RET_W ** -0.5, 0.1875, ((0, 4),)),
        "resid": normal_values(streams_of[7], (SEQUENCE_TOKENS, D), 1.0, 6.0, ((0, 32),)),
        "post_mix_gain": jnp.clip(1.0 + 0.18 * jax.random.normal(streams_of[8], (D,), jnp.float32), 0.1, 1.9),
        "pre_ffn_gain": jnp.clip(1.0 + 0.18 * jax.random.normal(streams_of[9], (D,), jnp.float32), 0.1, 1.9),
        "w_gate": normal_values(streams_of[10], (D, FF), D ** -0.5, 0.125, ((0, 8), (1, 4))),
        "w_up": normal_values(streams_of[11], (D, FF), D ** -0.5, 0.125, ((0, 8), (1, 4))),
        "w_down": normal_values(streams_of[12], (FF, D), FF ** -0.5, 0.078125, ((0, 4), (1, 8))),
        "post_ffn_gain": jnp.clip(1.0 + 0.18 * jax.random.normal(streams_of[13], (D,), jnp.float32), 0.1, 1.9),
    }


EPSILON = 1e-06

def rms_norm(values_in, gain_vec):
    widened = values_in.astype(jnp.float32)
    return widened * lax.rsqrt(lax.optimization_barrier(jnp.mean(widened * widened, axis=-1, keepdims=True)) + EPSILON) * gain_vec.astype(jnp.float32)

def block_step(carried, pieces):
    query_blk, key_blk, value_blk, decay_blk = pieces
    length = query_blk.shape[1]
    key_scale = query_blk.shape[2] ** (-0.5)
    query_wide = query_blk.astype(jnp.float32)
    key_wide = key_blk.astype(jnp.float32)
    value_wide = value_blk.astype(jnp.float32)
    cumulative = jnp.cumsum(decay_blk, axis=1)
    log_gap = cumulative[:, :, None] - cumulative[:, None, :]
    causal = lax.broadcasted_iota(jnp.int32, (length, length), 0) >= lax.broadcasted_iota(jnp.int32, (length, length), 1)
    weight = jnp.where(causal[None], jnp.exp(jnp.minimum(log_gap, 0.0)), 0.0)
    products = jnp.einsum('htd,hsd->hts', query_wide, key_wide)
    scores = lax.optimization_barrier((products * key_scale * weight).astype(jnp.bfloat16))
    within = jnp.einsum('hts,hsd->htd', scores.astype(jnp.float32), value_wide)
    carried_term = jnp.einsum('htd,hde->hte', query_wide, carried, precision=lax.Precision.HIGHEST) * jnp.exp(cumulative)[:, :, None]
    to_end = jnp.exp(cumulative[:, -1:] - cumulative) * key_scale
    scaled_keys = lax.optimization_barrier((key_wide * to_end[:, :, None]).astype(jnp.bfloat16))
    added = jnp.einsum('hsd,hse->hde', scaled_keys.astype(jnp.float32), value_wide)
    carried = jnp.exp(cumulative[:, -1])[:, None, None] * carried + added
    return (carried, within + carried_term)

def to_blocks(matrix, block_len, head_count):
    row_count = matrix.shape[0]
    return matrix.reshape(row_count // block_len, block_len, head_count, -1).transpose(0, 2, 1, 3)

def finish_heads(retention, gates, norm_gain):
    centered = retention - lax.optimization_barrier(jnp.mean(retention, axis=-1, keepdims=True))
    variance = lax.optimization_barrier(jnp.mean(centered * centered, axis=-1, keepdims=True))
    normed = centered * lax.rsqrt(variance + EPSILON) * norm_gain.astype(jnp.float32)[None]
    gate_vals = gates.astype(jnp.float32).reshape(normed.shape)
    return (jax.nn.silu(gate_vals) * normed).reshape(normed.shape[0], -1).astype(jnp.bfloat16)

def grouped_product(left, right, group_count):
    inner = left.shape[1] // group_count
    total = jnp.zeros((left.shape[0], right.shape[1]), jnp.float32)
    for group in range(group_count):
        part = jnp.dot(left[:, group * inner:(group + 1) * inner], right[group * inner:(group + 1) * inner], preferred_element_type=jnp.float32)
        total = total + part.astype(jnp.bfloat16).astype(jnp.float32)
    return total.astype(jnp.bfloat16)

def reference(queries, keys, values, gates, log_decay, norm_gain, out_weight, resid, post_mix_gain, pre_ffn_gain, w_gate, w_up, w_down, post_ffn_gain):
    block_count = SEQUENCE_TOKENS // BLOCK
    query_blocks = to_blocks(queries, BLOCK, RETENTION_HEADS)
    key_blocks = to_blocks(keys, BLOCK, RETENTION_HEADS)
    value_blocks = to_blocks(values, BLOCK, RETENTION_HEADS)
    decay_blocks = log_decay.reshape(block_count, BLOCK, RETENTION_HEADS).transpose(0, 2, 1)
    start_state = jnp.zeros((RETENTION_HEADS, HEAD_DIM, HEAD_DIM), jnp.float32)
    _, outputs = lax.scan(block_step, start_state, (query_blocks, key_blocks, value_blocks, decay_blocks))
    retention = outputs.transpose(0, 2, 1, 3).reshape(SEQUENCE_TOKENS, RETENTION_HEADS, HEAD_DIM)
    retained = finish_heads(retention, gates, norm_gain)
    mixed = grouped_product(retained, out_weight, N_TP)
    middle = (resid.astype(jnp.float32) + rms_norm(mixed, post_mix_gain)).astype(jnp.bfloat16)
    ffn_input = rms_norm(middle, pre_ffn_gain).astype(jnp.bfloat16)

    def ffn_rows(row_block):
        gate_act = jnp.dot(row_block, w_gate, preferred_element_type=jnp.float32)
        up_act = jnp.dot(row_block, w_up, preferred_element_type=jnp.float32)
        hidden = (jax.nn.silu(gate_act) * up_act).astype(jnp.bfloat16)
        return grouped_product(hidden, w_down, N_TP)
    branch = lax.map(ffn_rows, ffn_input.reshape(SEQUENCE_TOKENS // TOK_DEV, TOK_DEV, D)).reshape(SEQUENCE_TOKENS, D)
    return (middle.astype(jnp.float32) + rms_norm(branch, post_ffn_gain)).astype(jnp.bfloat16)
```

```python
import jax
import jax.numpy as jnp
from jax import lax
from jax.sharding import PartitionSpec as P


BLOCK = 512


EPSILON = 1e-06
LONGEST_RING = 8


def entering(decay, state):
    place = lax.axis_index("sp")
    head_count, head_dim, _ = state.shape
    decay_rows = jnp.broadcast_to(decay[:, None, None], (head_count, 16, head_dim))
    packed = jnp.concatenate([state, decay_rows], axis=1).astype(jnp.bfloat16)
    gathered = lax.all_gather(packed, "sp")

    def one(step, running):
        piece = lax.dynamic_index_in_dim(gathered, step, 0, False).astype(jnp.float32)
        return piece[:, head_dim : head_dim + 1, :] * running + piece[:, :head_dim]

    return lax.fori_loop(0, place, one, jnp.zeros_like(state))


def from_earlier(packed, distance):
    count = lax.axis_size("sp")
    return lax.ppermute(packed, "sp", [(i, i + distance) for i in range(count - distance)])


def entering_by_hops(decay, state):
    count = lax.axis_size("sp")
    head_count, head_dim, _ = state.shape
    decay_rows = jnp.broadcast_to(decay[:, None, None], (head_count, 8, head_dim))
    packed = jnp.concatenate([state, decay_rows], axis=1)
    near = from_earlier(packed, 1)
    far = from_earlier(packed, 2)
    factor = near[:, head_dim:]
    pair = jnp.concatenate(
        [factor[:, :1] * far[:, :head_dim] + near[:, :head_dim], factor * far[:, head_dim:]],
        axis=1,
    )
    total, factor = pair[:, :head_dim], pair[:, head_dim : head_dim + 1]
    for piece in [from_earlier(pair, distance) for distance in range(2, count, 2)]:
        total = total + factor * piece[:, :head_dim]
        factor = factor * piece[:, head_dim : head_dim + 1]
    return total


def ring_order(count):
    return list(range(0, count, 2)) + list(range(1, count, 2))[::-1]


def ring_gather(block, forward_steps, backward_steps):
    count = lax.axis_size("sp")
    order = ring_order(count)
    ahead = [(order[i], order[(i + 1) % count]) for i in range(count)]
    behind = [(b, a) for a, b in ahead]
    arrived = [(0, block)]
    up, down = block, block
    for step in range(1, max(forward_steps, backward_steps) + 1):
        if step <= forward_steps:
            up = lax.ppermute(up, "sp", ahead)
            arrived.append((-step, up))
        if step <= backward_steps:
            down = lax.ppermute(down, "sp", behind)
            arrived.append((step, down))
    return arrived


def owner_of(offset):
    count = lax.axis_size("sp")
    me = lax.axis_index("sp")
    half = (count + 1) // 2
    position = jnp.where(me % 2 == 0, me // 2, count - 1 - me // 2)
    there = (position + offset + count) % count
    return jnp.where(there < half, 2 * there, 2 * (count - 1 - there) + 1)


def rms_norm(values_in, gain_vec):
    widened = values_in.astype(jnp.float32)
    return (
        widened
        * lax.rsqrt(jnp.mean(widened * widened, axis=-1, keepdims=True) + EPSILON)
        * gain_vec
    )


def block_step(carried, pieces):
    query_blk, key_blk, value_blk, decay_blk = pieces
    length = query_blk.shape[1]
    key_scale = query_blk.shape[2] ** (-0.5)
    cumulative = jnp.cumsum(decay_blk, axis=1)
    log_gap = cumulative[:, :, None] - cumulative[:, None, :]
    causal = lax.broadcasted_iota(jnp.int32, (length, length), 0) >= lax.broadcasted_iota(
        jnp.int32, (length, length), 1
    )
    weight = jnp.where(causal[None], jnp.exp(jnp.minimum(log_gap, 0.0)), 0.0)
    products = jnp.einsum("htd,hsd->hts", query_blk, key_blk, preferred_element_type=jnp.float32)
    scores = (products * key_scale * weight).astype(jnp.bfloat16)
    within = jnp.einsum("hts,hsd->htd", scores, value_blk, preferred_element_type=jnp.float32)
    carried_term = (
        jnp.einsum(
            "htd,hde->hte", query_blk.astype(jnp.float32), carried, precision=lax.Precision.HIGHEST
        )
        * jnp.exp(cumulative)[:, :, None]
    )
    to_end = jnp.exp(cumulative[:, -1:] - cumulative) * key_scale
    scaled_keys = (key_blk.astype(jnp.float32) * to_end[:, :, None]).astype(jnp.bfloat16)
    added = jnp.einsum("hsd,hse->hde", scaled_keys, value_blk, preferred_element_type=jnp.float32)
    carried = jnp.exp(cumulative[:, -1])[:, None, None] * carried + added
    return (carried, within + carried_term)


def to_blocks(matrix, block_len, head_count):
    row_count = matrix.shape[0]
    return matrix.reshape(row_count // block_len, block_len, head_count, -1).transpose(0, 2, 1, 3)


def finish_heads(retention, gates, norm_gain):
    centered = retention - jnp.mean(retention, axis=-1, keepdims=True)
    variance = jnp.mean(centered * centered, axis=-1, keepdims=True)
    normed = centered * lax.rsqrt(variance + EPSILON) * norm_gain[None]
    gate_vals = gates.astype(jnp.float32).reshape(normed.shape)
    return (jax.nn.silu(gate_vals) * normed).reshape(normed.shape[0], -1).astype(jnp.bfloat16)


def ring_feed_forward(rows, gate_blocks, up_blocks, down_blocks, shape):
    depth = gate_blocks[0][1].shape[0]
    width = down_blocks[0][1].shape[1]
    half = (len(gate_blocks) + 1) // 2

    def project(blocks):
        total = None
        for some in (blocks[:half], blocks[half:]):
            if not some:
                continue
            columns = jnp.concatenate(
                [
                    lax.dynamic_slice_in_dim(rows, owner_of(offset) * depth, depth, 1)
                    for offset, _ in some
                ],
                axis=1,
            )
            weight = jnp.concatenate([block for _, block in some], axis=0)
            part = jnp.dot(columns, weight, preferred_element_type=jnp.float32)
            total = part if total is None else total + part
        return total

    gate_act = project(gate_blocks)
    up_act = project(up_blocks)
    hidden = (jax.nn.silu(gate_act) * up_act).astype(jnp.bfloat16)
    branch = jnp.zeros(shape, jnp.bfloat16)
    for part_no, some in enumerate((down_blocks[:half], down_blocks[half:])):
        if not some:
            continue
        wide = jnp.concatenate([block for _, block in some], axis=1)
        part = jnp.dot(hidden, wide, preferred_element_type=jnp.float32).astype(jnp.bfloat16)
        if part_no == 0:
            piece = lax.psum_scatter(part, "tp", scatter_dimension=0, tiled=True)
        else:
            shares = part.reshape(lax.axis_size("tp"), shape[0], -1)
            shares = lax.all_to_all(shares, "tp", split_axis=0, concat_axis=0, tiled=True)
            piece = jnp.sum(shares.astype(jnp.float32), axis=0).astype(jnp.bfloat16)
        for slot, (offset, _) in enumerate(some):
            branch = lax.dynamic_update_slice_in_dim(
                branch, piece[:, slot * width : (slot + 1) * width], owner_of(offset) * width, 1
            )
    return branch


def per_device(
    queries,
    keys,
    values,
    gates,
    log_decay,
    norm_gain,
    out_weight,
    resid,
    post_mix_gain,
    pre_ffn_gain,
    w_gate,
    w_up,
    w_down,
    post_ffn_gain,
):
    ring = lax.axis_size("sp")
    fewer = (ring - 1) // 2
    more = ring - 1 - fewer
    short = ring <= LONGEST_RING
    if short:
        gate_blocks = ring_gather(w_gate, more, fewer)
        up_blocks = ring_gather(w_up, fewer, more)
        down_blocks = ring_gather(w_down, more, fewer)
    row_count = queries.shape[0]
    head_count = log_decay.shape[1]
    head_dim = queries.shape[1] // head_count
    block_count = row_count // BLOCK
    query_blocks = to_blocks(queries, BLOCK, head_count)
    key_blocks = to_blocks(keys, BLOCK, head_count)
    value_blocks = to_blocks(values, BLOCK, head_count)
    decay_blocks = log_decay.reshape(block_count, BLOCK, head_count).transpose(0, 2, 1)
    start_state = jnp.zeros((head_count, head_dim, head_dim), jnp.float32)
    local_state, outputs = lax.scan(
        block_step, start_state, (query_blocks, key_blocks, value_blocks, decay_blocks)
    )
    retention = outputs.transpose(0, 2, 1, 3).reshape(row_count, head_count, head_dim)
    cumulative = jnp.cumsum(log_decay, axis=0)
    local_decay = jnp.exp(cumulative[-1])
    incoming = (entering_by_hops if short else entering)(local_decay, local_state)
    query_rows = queries.reshape(row_count, head_count, head_dim).astype(jnp.float32)
    retention = (
        retention
        + jnp.einsum("thd,hde->the", query_rows, incoming, precision=lax.Precision.HIGHEST)
        * jnp.exp(cumulative)[:, :, None]
    )
    retained = finish_heads(retention, gates, norm_gain)
    quarter = resid.shape[0]
    regrouped = lax.all_to_all(retained, "tp", split_axis=0, concat_axis=1, tiled=True)
    group_rows = out_weight.shape[0]
    empty_mix = jnp.zeros((quarter, out_weight.shape[1]), jnp.float32)
    running = empty_mix
    shard_piece = lax.all_gather(out_weight, "tp", axis=0, tiled=True)
    for offset in range(shard_piece.shape[0] // group_rows):
        columns = lax.dynamic_slice_in_dim(regrouped, offset * group_rows, group_rows, 1)
        part = jnp.dot(
            columns,
            shard_piece[offset * group_rows : (offset + 1) * group_rows],
            preferred_element_type=jnp.float32,
        )
        running = running + part.astype(jnp.bfloat16).astype(jnp.float32)
    mixed = running
    mixed = mixed.astype(jnp.bfloat16)
    middle = (resid.astype(jnp.float32) + rms_norm(mixed, post_mix_gain)).astype(jnp.bfloat16)
    ffn_input = rms_norm(middle, pre_ffn_gain).astype(jnp.bfloat16)
    gathered = lax.all_gather(ffn_input, "tp", axis=0, tiled=True)
    if not short:
        gate_act = jnp.dot(
            gathered,
            lax.all_gather(w_gate, "sp", axis=0, tiled=True),
            preferred_element_type=jnp.float32,
        )
        up_act = jnp.dot(
            gathered,
            lax.all_gather(w_up, "sp", axis=0, tiled=True),
            preferred_element_type=jnp.float32,
        )
        hidden = (jax.nn.silu(gate_act) * up_act).astype(jnp.bfloat16)
        down_full = lax.all_gather(w_down, "sp", axis=1, tiled=True)
        partial = jnp.dot(hidden, down_full, preferred_element_type=jnp.float32)
        branch = lax.psum_scatter(
            partial.astype(jnp.bfloat16), "tp", scatter_dimension=0, tiled=True
        )
    else:
        branch = ring_feed_forward(gathered, gate_blocks, up_blocks, down_blocks, resid.shape)
    return (middle.astype(jnp.float32) + rms_norm(branch, post_ffn_gain)).astype(jnp.bfloat16)


def solution(mesh):
    in_specs = (
        P("sp", "tp"),
        P("sp", "tp"),
        P("sp", "tp"),
        P("sp", "tp"),
        P("sp", "tp"),
        P("tp", None),
        P("tp", None),
        P(("sp", "tp"), None),
        P(),
        P(),
        P("sp", "tp"),
        P("sp", "tp"),
        P("tp", "sp"),
        P(),
    )
    out_specs = P(("sp", "tp"), None)

    return jax.shard_map(
        per_device, mesh=mesh, in_specs=in_specs, out_specs=out_specs, check_vma=False
    )
```

```python
import jax
import jax.numpy as jnp
from jax import lax
from jax.sharding import PartitionSpec as P


BLOCK = 512


EPSILON = 1e-06
LONGEST_RING = 8


def entering(decay, state):
    place = lax.axis_index("sp")
    head_count, head_dim, _ = state.shape
    decay_rows = jnp.broadcast_to(decay[:, None, None], (head_count, 16, head_dim))
    packed = jnp.concatenate([state, decay_rows], axis=1).astype(jnp.bfloat16)
    gathered = lax.all_gather(packed, "sp")

    def one(step, running):
        piece = lax.dynamic_index_in_dim(gathered, step, 0, False).astype(jnp.float32)
        return piece[:, head_dim : head_dim + 1, :] * running + piece[:, :head_dim]

    return lax.fori_loop(0, place, one, jnp.zeros_like(state))


def from_earlier(packed, distance):
    count = lax.axis_size("sp")
    return lax.ppermute(packed, "sp", [(i, i + distance) for i in range(count - distance)])


def entering_by_hops(decay, state):
    count = lax.axis_size("sp")
    head_count, head_dim, _ = state.shape
    decay_rows = jnp.broadcast_to(decay[:, None, None], (head_count, 8, head_dim))
    packed = jnp.concatenate([state, decay_rows], axis=1)
    near = from_earlier(packed, 1)
    far = from_earlier(packed, 2)
    factor = near[:, head_dim:]
    pair = jnp.concatenate(
        [factor[:, :1] * far[:, :head_dim] + near[:, :head_dim], factor * far[:, head_dim:]],
        axis=1,
    )
    total, factor = pair[:, :head_dim], pair[:, head_dim : head_dim + 1]
    for piece in [from_earlier(pair, distance) for distance in range(2, count, 2)]:
        total = total + factor * piece[:, :head_dim]
        factor = factor * piece[:, head_dim : head_dim + 1]
    return total


def ring_order(count):
    return list(range(0, count, 2)) + list(range(1, count, 2))[::-1]


def ring_gather(block, forward_steps, backward_steps):
    count = lax.axis_size("sp")
    order = ring_order(count)
    ahead = [(order[i], order[(i + 1) % count]) for i in range(count)]
    behind = [(b, a) for a, b in ahead]
    arrived = [(0, block)]
    up, down = block, block
    for step in range(1, max(forward_steps, backward_steps) + 1):
        if step <= forward_steps:
            up = lax.ppermute(up, "sp", ahead)
            arrived.append((-step, up))
        if step <= backward_steps:
            down = lax.ppermute(down, "sp", behind)
            arrived.append((step, down))
    return arrived


def owner_of(offset):
    count = lax.axis_size("sp")
    me = lax.axis_index("sp")
    half = (count + 1) // 2
    position = jnp.where(me % 2 == 0, me // 2, count - 1 - me // 2)
    there = (position + offset + count) % count
    return jnp.where(there < half, 2 * there, 2 * (count - 1 - there) + 1)


def rms_norm(values_in, gain_vec):
    widened = values_in.astype(jnp.float32)
    return (
        widened
        * lax.rsqrt(jnp.mean(widened * widened, axis=-1, keepdims=True) + EPSILON)
        * gain_vec
    )


def block_step(carried, pieces):
    query_blk, key_blk, value_blk, decay_blk = pieces
    length = query_blk.shape[1]
    key_scale = query_blk.shape[2] ** (-0.5)
    cumulative = jnp.cumsum(decay_blk, axis=1)
    log_gap = cumulative[:, :, None] - cumulative[:, None, :]
    causal = lax.broadcasted_iota(jnp.int32, (length, length), 0) >= lax.broadcasted_iota(
        jnp.int32, (length, length), 1
    )
    weight = jnp.where(causal[None], jnp.exp(jnp.minimum(log_gap, 0.0)), 0.0)
    products = jnp.einsum("htd,hsd->hts", query_blk, key_blk, preferred_element_type=jnp.float32)
    scores = (products * key_scale * weight).astype(jnp.bfloat16)
    within = jnp.einsum("hts,hsd->htd", scores, value_blk, preferred_element_type=jnp.float32)
    carried_term = (
        jnp.einsum(
            "htd,hde->hte", query_blk.astype(jnp.float32), carried, precision=lax.Precision.HIGHEST
        )
        * jnp.exp(cumulative)[:, :, None]
    )
    to_end = jnp.exp(cumulative[:, -1:] - cumulative) * key_scale
    scaled_keys = (key_blk.astype(jnp.float32) * to_end[:, :, None]).astype(jnp.bfloat16)
    added = jnp.einsum("hsd,hse->hde", scaled_keys, value_blk, preferred_element_type=jnp.float32)
    carried = jnp.exp(cumulative[:, -1])[:, None, None] * carried + added
    return (carried, within + carried_term)


def to_blocks(matrix, block_len, head_count):
    row_count = matrix.shape[0]
    return matrix.reshape(row_count // block_len, block_len, head_count, -1).transpose(0, 2, 1, 3)


def finish_heads(retention, gates, norm_gain):
    centered = retention - jnp.mean(retention, axis=-1, keepdims=True)
    variance = jnp.mean(centered * centered, axis=-1, keepdims=True)
    normed = centered * lax.rsqrt(variance + EPSILON) * norm_gain[None]
    gate_vals = gates.astype(jnp.float32).reshape(normed.shape)
    return (jax.nn.silu(gate_vals) * normed).reshape(normed.shape[0], -1).astype(jnp.bfloat16)


def share_sum(part, row_count):
    count = lax.axis_size("tp")
    if count != 4:
        return lax.psum_scatter(part, "tp", scatter_dimension=0, tiled=True)
    me = lax.axis_index("tp")
    high, low = me // 2, me % 2
    shares = part.reshape(2, 2, row_count, -1)

    def swap(block, bit):
        return lax.ppermute(block, "tp", [(i, i ^ bit) for i in range(count)])

    def pick(block, index, dim):
        return lax.dynamic_index_in_dim(block, index, dim, False)

    nearer = swap(pick(shares, 1 - low, 1), 1).astype(jnp.float32)
    pair = pick(shares, low, 1).astype(jnp.float32) + nearer
    farther = swap(pick(pair, 1 - high, 0).astype(jnp.bfloat16), 2).astype(jnp.float32)
    return (pick(pair, high, 0) + farther).astype(jnp.bfloat16)


def ring_feed_forward(rows, gate_blocks, up_blocks, down_blocks, shape):
    depth = gate_blocks[0][1].shape[0]
    width = down_blocks[0][1].shape[1]
    half = (len(gate_blocks) + 1) // 2

    def project(blocks):
        total = None
        for some in (blocks[:half], blocks[half:]):
            if not some:
                continue
            columns = jnp.concatenate(
                [
                    lax.dynamic_slice_in_dim(rows, owner_of(offset) * depth, depth, 1)
                    for offset, _ in some
                ],
                axis=1,
            )
            weight = jnp.concatenate([block for _, block in some], axis=0)
            part = jnp.dot(columns, weight, preferred_element_type=jnp.float32)
            total = part if total is None else total + part
        return total

    gate_act = project(gate_blocks)
    up_act = project(up_blocks)
    hidden = (jax.nn.silu(gate_act) * up_act).astype(jnp.bfloat16)
    branch = jnp.zeros(shape, jnp.bfloat16)
    for some in (down_blocks[:half], down_blocks[half:]):
        if not some:
            continue
        wide = jnp.concatenate([block for _, block in some], axis=1)
        part = jnp.dot(hidden, wide, preferred_element_type=jnp.float32).astype(jnp.bfloat16)
        piece = share_sum(part, shape[0])
        for slot, (offset, _) in enumerate(some):
            branch = lax.dynamic_update_slice_in_dim(
                branch, piece[:, slot * width : (slot + 1) * width], owner_of(offset) * width, 1
            )
    return branch


def per_device(
    queries,
    keys,
    values,
    gates,
    log_decay,
    norm_gain,
    out_weight,
    resid,
    post_mix_gain,
    pre_ffn_gain,
    w_gate,
    w_up,
    w_down,
    post_ffn_gain,
):
    ring = lax.axis_size("sp")
    fewer = (ring - 1) // 2
    more = ring - 1 - fewer
    short = ring <= LONGEST_RING
    if short:
        gate_blocks = ring_gather(w_gate, more, fewer)
        up_blocks = ring_gather(w_up, fewer, more)
        down_blocks = ring_gather(w_down, more, fewer)
    row_count = queries.shape[0]
    head_count = log_decay.shape[1]
    head_dim = queries.shape[1] // head_count
    block_count = row_count // BLOCK
    query_blocks = to_blocks(queries, BLOCK, head_count)
    key_blocks = to_blocks(keys, BLOCK, head_count)
    value_blocks = to_blocks(values, BLOCK, head_count)
    decay_blocks = log_decay.reshape(block_count, BLOCK, head_count).transpose(0, 2, 1)
    start_state = jnp.zeros((head_count, head_dim, head_dim), jnp.float32)
    local_state, outputs = lax.scan(
        block_step, start_state, (query_blocks, key_blocks, value_blocks, decay_blocks)
    )
    retention = outputs.transpose(0, 2, 1, 3).reshape(row_count, head_count, head_dim)
    cumulative = jnp.cumsum(log_decay, axis=0)
    local_decay = jnp.exp(cumulative[-1])
    incoming = (entering_by_hops if short else entering)(local_decay, local_state)
    query_rows = queries.reshape(row_count, head_count, head_dim).astype(jnp.float32)
    retention = (
        retention
        + jnp.einsum("thd,hde->the", query_rows, incoming, precision=lax.Precision.HIGHEST)
        * jnp.exp(cumulative)[:, :, None]
    )
    retained = finish_heads(retention, gates, norm_gain)
    quarter = resid.shape[0]
    regrouped = lax.all_to_all(retained, "tp", split_axis=0, concat_axis=1, tiled=True)
    group_rows = out_weight.shape[0]
    empty_mix = jnp.zeros((quarter, out_weight.shape[1]), jnp.float32)
    running = empty_mix
    shard_piece = lax.all_gather(out_weight, "tp", axis=0, tiled=True)
    for offset in range(shard_piece.shape[0] // group_rows):
        columns = lax.dynamic_slice_in_dim(regrouped, offset * group_rows, group_rows, 1)
        part = jnp.dot(
            columns,
            shard_piece[offset * group_rows : (offset + 1) * group_rows],
            preferred_element_type=jnp.float32,
        )
        running = running + part.astype(jnp.bfloat16).astype(jnp.float32)
    mixed = running
    mixed = mixed.astype(jnp.bfloat16)
    middle = (resid.astype(jnp.float32) + rms_norm(mixed, post_mix_gain)).astype(jnp.bfloat16)
    ffn_input = rms_norm(middle, pre_ffn_gain).astype(jnp.bfloat16)
    gathered = lax.all_gather(ffn_input, "tp", axis=0, tiled=True)
    if not short:
        gate_act = jnp.dot(
            gathered,
            lax.all_gather(w_gate, "sp", axis=0, tiled=True),
            preferred_element_type=jnp.float32,
        )
        up_act = jnp.dot(
            gathered,
            lax.all_gather(w_up, "sp", axis=0, tiled=True),
            preferred_element_type=jnp.float32,
        )
        hidden = (jax.nn.silu(gate_act) * up_act).astype(jnp.bfloat16)
        down_full = lax.all_gather(w_down, "sp", axis=1, tiled=True)
        partial = jnp.dot(hidden, down_full, preferred_element_type=jnp.float32)
        branch = lax.psum_scatter(
            partial.astype(jnp.bfloat16), "tp", scatter_dimension=0, tiled=True
        )
    else:
        branch = ring_feed_forward(gathered, gate_blocks, up_blocks, down_blocks, resid.shape)
    return (middle.astype(jnp.float32) + rms_norm(branch, post_ffn_gain)).astype(jnp.bfloat16)


def solution(mesh):
    in_specs = (
        P("sp", "tp"),
        P("sp", "tp"),
        P("sp", "tp"),
        P("sp", "tp"),
        P("sp", "tp"),
        P("tp", None),
        P("tp", None),
        P(("sp", "tp"), None),
        P(),
        P(),
        P("sp", "tp"),
        P("sp", "tp"),
        P("tp", "sp"),
        P(),
    )
    out_specs = P(("sp", "tp"), None)

    return jax.shard_map(
        per_device, mesh=mesh, in_specs=in_specs, out_specs=out_specs, check_vma=False
    )
```
